32 devices in a mesh: sp: 8 (over z, y), tp: 4 (over x, core).
Axes of the slice: x: 2, y: 2, z: 4, core: 2. Of those that a mesh axis runs over, the one named last changes fastest.
Arguments:
- tokens: bfloat16 [8192, 2048], P('sp'), may hold values from -6 to 6
- norm_gain: bfloat16 [2048], replicated, may hold values from 0.099609375 to 1.8984375
- query_weight: bfloat16 [2048, 2048], P(None, 'tp'), may hold values from -0.125 to 0.125
- key_weight: bfloat16 [2048, 512], P(None, 'tp'), may hold values from -0.125 to 0.125
- value_weight: bfloat16 [2048, 512], P(None, 'tp'), may hold values from -0.125 to 0.125
- query_gain: float32 [64], replicated, may hold values from 1 to 14
- key_gain: float32 [64], replicated, may hold values from 1 to 14
- sink_logit: float32 [32], P('tp'), may hold values from 4 to 10
- gate_weight: bfloat16 [2048, 4096], P(None, 'tp'), may hold values from -0.125 to 0.125
- inner_weight: bfloat16 [2048, 4096], P(None, 'tp'), may hold values from -0.125 to 0.125
- input_map: bfloat16 [2048, 1024], P(None, 'tp'), may hold values from -0.125 to 0.125
- output_map: bfloat16 [2048, 1024], P(None, 'tp'), may hold values from -0.125 to 0.125
- step_weight: bfloat16 [2048, 2, 64], P(None, None, 'tp'), may hold values from -0.125 to 0.125
- conv_inner: bfloat16 [5, 4096], P(None, 'tp'), may hold values from -2.5 to 2.5
- conv_pair: bfloat16 [5, 2, 1024], P(None, None, 'tp'), may hold values from -2.5 to 2.5
- decay_rate: float32 [2, 64], P(None, 'tp'), may hold values from 3.6621094e-06 to 0.05
- decay_jump: float32 [8192, 2, 64], P('sp', None, 'tp'), may hold values from -1.4001709 to 0
- inner_gain: bfloat16 [4096], P('tp'), may hold values from 0.099609375 to 1.8984375
- attn_out_weight: bfloat16 [2048, 2048], P('tp'), may hold values from -0.25 to 0.25
- ssm_out_weight: bfloat16 [4096, 2048], P('tp'), may hold values from -0.09375 to 0.09375
Outputs:
- mixed: bfloat16 [8192, 2048], P(('sp', 'tp'))
The draws below stay inside these ranges and needn't reach their ends.
All inputs are finite; a program needn't handle non-finite values.
Results may differ from the reference program's by a relative error of at most 0.025.
The reference program's roundings to bfloat16 on the way count: a program that leaves them out, or rounds other values in their place, can miss the bound.
Values may be sent and summed in bfloat16 or wider, within the bound.
A program may use at most 128 MiB of HBM per device.

```python
import math
import jax
import jax.numpy as jnp
from jax import lax

MODEL_WIDTH = 2048
HEAD_SIZE = 64
QUERY_HEADS = 32
KEY_HEADS = 8
SSM_INNER = 4096
SSM_GROUPS = 8
STATE_SIZE = 128
CONV_TAPS = 5
WINDOW = 128
BLOCK_ROWS = 256
LOCAL_TOKENS = 1024
DUALITY_CHANNELS = 64
ORDERED_ENTRIES = 8192
N_TP = 4


def draw_query_gain(key, part):
    gain_key = jax.random.fold_in(key, 11)
    return jax.random.uniform(gain_key, (HEAD_SIZE,), jnp.float32, 1.0, 2.0)


def draw_key_gain(key, part):
    gain_key = jax.random.fold_in(key, 17)
    return jax.random.uniform(gain_key, (HEAD_SIZE,), jnp.float32, 1.0, 2.0)


def draw_decay_rate(key, part):
    coin_key, fast_key, slow_key = jax.random.split(jax.random.fold_in(key, 23), 3)
    shape_pair = (2, DUALITY_CHANNELS)
    fast_rate = jnp.exp(jax.random.uniform(fast_key, shape_pair, jnp.float32, math.log(0.015), math.log(0.05)))
    slow_rate = jnp.exp(jax.random.uniform(slow_key, shape_pair, jnp.float32, math.log(0.05 / ORDERED_ENTRIES), math.log(0.3 / ORDERED_ENTRIES)))
    picked = jax.random.bernoulli(coin_key, 0.5, shape_pair)
    return jnp.where(picked, fast_rate, slow_rate)


def draw_decay_jump(key, part):
    pace_key, spot_key, depth_key = jax.random.split(jax.random.fold_in(key, 37), 3)
    columns = 2 * DUALITY_CHANNELS
    blocks = ORDERED_ENTRIES // BLOCK_ROWS
    pace = jax.random.uniform(pace_key, (blocks, 1, columns), jnp.float32, 0.0, 1.4 / ORDERED_ENTRIES)
    increment_matrix_lines = jnp.broadcast_to(pace, (blocks, BLOCK_ROWS, columns)).reshape(ORDERED_ENTRIES, columns)
    drawn_locations = jax.random.randint(spot_key, (2, columns), 0, ORDERED_ENTRIES, dtype=jnp.int32)
    stack_level_count = jnp.log(jax.random.uniform(depth_key, (2, columns), jnp.float32, 0.5, 0.8))
    entry_ordinal = jnp.arange(ORDERED_ENTRIES, dtype=jnp.int32)[:, None]
    cluster_bunches = jnp.where(entry_ordinal == drawn_locations[0][None, :], stack_level_count[0][None, :], 0.0)
    cluster_bunches = cluster_bunches + jnp.where(entry_ordinal == drawn_locations[1][None, :], stack_level_count[1][None, :], 0.0)
    return (cluster_bunches - increment_matrix_lines).reshape(ORDERED_ENTRIES, 2, DUALITY_CHANNELS)


def shard_levels(key, dims, shards, smallest, high):
    loudness, own = 1.0, jax.random.fold_in(key, 6)
    for dim, shards_of in shards:
        draws = jnp.exp(jax.random.uniform(jax.random.fold_in(own, dim), (shards_of,), jnp.float32, smallest / len(shards), high / len(shards)))
        loudness = loudness * jnp.repeat(draws, dims[dim] // shards_of).reshape([-1 if axis == dim else 1 for axis in range(len(dims))])
    return loudness


def bell_draw(key, extent, width, limit, shards=(), kind=jnp.bfloat16):
    values = jax.random.normal(key, extent, jnp.float32) * width
    if len(shards) > 0:
        values = shard_levels(key, extent, shards, -0.22, 0.18) * values
    return jnp.clip(values, min=-limit, max=limit).astype(kind)


def setup_inputs(seed: int = 0) -> dict:
    splits = jax.random.split(jax.random.key(seed), 21)
    return {
        "tokens": bell_draw(splits[0], (ORDERED_ENTRIES, MODEL_WIDTH), 1.0, 6.0, ((0, 8),)),
        "norm_gain": jnp.clip(1.0 + 0.18 * jax.random.normal(splits[1], (MODEL_WIDTH,), jnp.float32), 0.099609375, 1.8984375).astype(jnp.bfloat16),
        "query_weight": bell_draw(splits[2], (MODEL_WIDTH, QUERY_HEADS * HEAD_SIZE), MODEL_WIDTH ** -0.5, 0.125, ((1, 4),)),
        "key_weight": bell_draw(splits[3], (MODEL_WIDTH, KEY_HEADS * HEAD_SIZE), MODEL_WIDTH ** -0.5, 0.125, ((1, 4),)),
        "value_weight": bell_draw(splits[4], (MODEL_WIDTH, KEY_HEADS * HEAD_SIZE), MODEL_WIDTH ** -0.5, 0.125, ((1, 4),)),
        "query_gain": draw_query_gain(jax.random.fold_in(splits[20], 71), 0),
        "key_gain": draw_key_gain(jax.random.fold_in(splits[20], 71), 0),
        "sink_logit": jnp.clip(4.0 + 6.0 * jax.random.uniform(splits[7], (QUERY_HEADS,), jnp.float32) ** shard_levels(splits[7], (QUERY_HEADS,), ((0, 4),), -0.2, 0.2), 4.0, 10.0),
        "gate_weight": bell_draw(splits[8], (MODEL_WIDTH, SSM_INNER), MODEL_WIDTH ** -0.5, 0.125, ((1, 4),)),
        "inner_weight": bell_draw(splits[9], (MODEL_WIDTH, SSM_INNER), MODEL_WIDTH ** -0.5, 0.125, ((1, 4),)),
        "input_map": bell_draw(splits[10], (MODEL_WIDTH, SSM_GROUPS * STATE_SIZE), MODEL_WIDTH ** -0.5, 0.125, ((1, 4),)),
        "output_map": bell_draw(splits[11], (MODEL_WIDTH, SSM_GROUPS * STATE_SIZE), MODEL_WIDTH ** -0.5, 0.125, ((1, 4),)),
        "step_weight": bell_draw(splits[12], (MODEL_WIDTH, 2, DUALITY_CHANNELS), MODEL_WIDTH ** -0.5, 0.125, ((2, 4),)),
        "conv_inner": bell_draw(splits[13], (CONV_TAPS, SSM_INNER), CONV_TAPS ** -0.5, 2.5, ((1, 4),)),
        "conv_pair": bell_draw(splits[14], (CONV_TAPS, 2, SSM_GROUPS * STATE_SIZE), CONV_TAPS ** -0.5, 2.5, ((2, 4),)),
        "decay_rate": draw_decay_rate(jax.random.fold_in(splits[20], 71), 0),
        "decay_jump": draw_decay_jump(jax.random.fold_in(splits[20], 71), 0),
        "inner_gain": jnp.clip(1.0 + 0.18 * jax.random.normal(splits[17], (SSM_INNER,), jnp.float32), 0.099609375, 1.8984375).astype(jnp.bfloat16),
        "attn_out_weight": bell_draw(splits[18], (QUERY_HEADS * HEAD_SIZE, MODEL_WIDTH), (QUERY_HEADS * HEAD_SIZE // 4) ** -0.5, 0.25, ((0, 4),)),
        "ssm_out_weight": bell_draw(splits[19], (SSM_INNER, MODEL_WIDTH), SSM_INNER ** -0.5, 0.09375, ((0, 4),)),
    }


NORM_EPS = 1e-05
ROPE_BASE = 500000.0
NEG_FILL = -1e+30

def rms_rows(values, scales):
    return values * lax.rsqrt(lax.optimization_barrier(jnp.mean(values * values, axis=-1, keepdims=True)) + NORM_EPS) * scales

def rotate(head_rows, positions):
    head_size = head_rows.shape[-1]
    half_size = head_size // 2
    frequency = ROPE_BASE ** (-jnp.arange(0, head_size, 2, dtype=jnp.float32) / head_size)
    angles = positions.astype(jnp.float32)[:, None] * frequency
    cosine = jnp.cos(angles)[:, None, :]
    sine_part = jnp.sin(angles)[:, None, :]
    first_half = head_rows[..., :half_size]
    second_half = head_rows[..., half_size:]
    return jnp.concatenate([first_half * cosine - second_half * sine_part, second_half * cosine + first_half * sine_part], axis=-1)

def attend(query, keyed, value, sink_logit):
    seq_total = query.shape[0]
    group_ratio = QUERY_HEADS // KEY_HEADS
    qblock = 512 if LOCAL_TOKENS % 512 == 0 else LOCAL_TOKENS
    key_reach = qblock + 2 * WINDOW
    rim_pad = ((WINDOW, WINDOW), (0, 0), (0, 0))
    padded_keys = jnp.pad(keyed, rim_pad)
    padded_values = jnp.pad(value, rim_pad)
    sink_table = sink_logit.astype(jnp.float32).reshape(KEY_HEADS, group_ratio)[:, :, None, None]

    def one_block(block_index):
        first_row = block_index * qblock
        block_query = lax.dynamic_slice_in_dim(query, first_row, qblock, 0)
        block_query = block_query.reshape(qblock, KEY_HEADS, group_ratio, HEAD_SIZE)
        key_part = lax.dynamic_slice_in_dim(padded_keys, first_row, key_reach, 0)
        value_part = lax.dynamic_slice_in_dim(padded_values, first_row, key_reach, 0)
        scores = jnp.einsum('qkrd,skd->krqs', block_query.astype(jnp.float32), key_part.astype(jnp.float32)) * HEAD_SIZE ** (-0.5)
        query_pos = first_row + jnp.arange(qblock, dtype=jnp.int32)
        key_pos = first_row - WINDOW + jnp.arange(key_reach, dtype=jnp.int32)
        allowed = (jnp.abs(query_pos[:, None] - key_pos[None, :]) <= WINDOW) & (key_pos[None, :] >= 0) & (key_pos[None, :] < seq_total)
        scores = jnp.where(allowed, scores, NEG_FILL)
        ceiling = jnp.maximum(lax.optimization_barrier(jnp.max(scores, axis=-1, keepdims=True)), sink_table)
        raised = jnp.exp(scores - ceiling)
        weights = raised / (lax.optimization_barrier(jnp.sum(raised, axis=-1, keepdims=True)) + jnp.exp(sink_table - ceiling))
        weights = lax.optimization_barrier(weights.astype(jnp.bfloat16))
        mixed_rows = jnp.einsum('krqs,skd->qkrd', weights.astype(jnp.float32), value_part.astype(jnp.float32))
        return mixed_rows.astype(jnp.bfloat16).reshape(qblock, QUERY_HEADS * HEAD_SIZE)
    blocks_out = lax.map(one_block, jnp.arange(seq_total // qblock, dtype=jnp.int32))
    return blocks_out.reshape(seq_total, QUERY_HEADS * HEAD_SIZE)

def ssd_pass(scaled, log_decay, in_state, out_state):
    seq_total, groups_all, ssm_ratio, head_size = scaled.shape
    state_size = in_state.shape[-1]
    blocks = seq_total // BLOCK_ROWS
    scaled_blocks = scaled.reshape(blocks, BLOCK_ROWS, groups_all, ssm_ratio, head_size)
    decay_blocks = log_decay.reshape(blocks, BLOCK_ROWS, groups_all, ssm_ratio)
    in_blocks = in_state.reshape(blocks, BLOCK_ROWS, groups_all, state_size)
    out_blocks = out_state.reshape(blocks, BLOCK_ROWS, groups_all, state_size)
    row_order = jnp.arange(BLOCK_ROWS)
    lower_mask = row_order[:, None] >= row_order[None, :]
    highest_precision = lax.Precision.HIGHEST

    def advance(carried, block_parts):
        local_scaled, decay_here, local_input, out_here = block_parts
        inside = jnp.cumsum(jnp.transpose(decay_here, (1, 2, 0)), axis=-1)
        weights_in = jnp.exp(jnp.where(lower_mask, inside[..., :, None] - inside[..., None, :], -jnp.inf))
        intersection = jnp.einsum('sgn,tgn->gst', out_here, local_input, precision=highest_precision)
        within = jnp.einsum('gst,grst,tgrp->sgrp', intersection, weights_in, local_scaled, precision=highest_precision)
        across = jnp.einsum('sgn,grpn,grs->sgrp', out_here, carried, jnp.exp(inside), precision=highest_precision)
        remaining_length = jnp.exp(inside[..., -1:] - inside)
        fresh_state = jnp.einsum('dle,lwd,dlwu->lwue', local_input, remaining_length, local_scaled, precision=highest_precision)
        updated = jnp.exp(inside[..., -1])[..., None, None] * carried + fresh_state
        return (updated, within + across)
    start_state = jnp.zeros((groups_all, ssm_ratio, head_size, state_size), jnp.float32)
    unused, outputs = lax.scan(advance, start_state, (scaled_blocks, decay_blocks, in_blocks, out_blocks))
    return outputs.reshape(seq_total, groups_all, ssm_ratio, head_size)

def reference(tokens, norm_gain, query_weight, key_weight, value_weight, query_gain, key_gain, sink_logit, gate_weight, inner_weight, input_map, output_map, step_weight, conv_inner, conv_pair, decay_rate, decay_jump, inner_gain, attn_out_weight, ssm_out_weight):
    seq_total = tokens.shape[0]
    positions = jnp.arange(seq_total, dtype=jnp.int32)
    normed = rms_rows(tokens.astype(jnp.float32), norm_gain.astype(jnp.float32)).astype(jnp.bfloat16)

    def project(weight):
        result = jnp.dot(normed, weight, preferred_element_type=jnp.float32)
        return lax.optimization_barrier(result.astype(jnp.bfloat16))
    query = project(query_weight).reshape(seq_total, QUERY_HEADS, HEAD_SIZE)
    keyed = project(key_weight).reshape(seq_total, KEY_HEADS, HEAD_SIZE)
    value = project(value_weight).reshape(seq_total, KEY_HEADS, HEAD_SIZE)
    query = rotate(rms_rows(query.astype(jnp.float32), query_gain), positions)
    query = lax.optimization_barrier(query.astype(jnp.bfloat16))
    keyed = rotate(rms_rows(keyed.astype(jnp.float32), key_gain), positions)
    keyed = lax.optimization_barrier(keyed.astype(jnp.bfloat16))
    attn_out = attend(query, keyed, value, sink_logit)
    ssm_ratio = DUALITY_CHANNELS // SSM_GROUPS
    gate_rows = project(gate_weight)
    carried_in = jnp.concatenate([project(inner_weight), project(input_map), project(output_map)], axis=1)
    carried_in = carried_in.astype(jnp.float32)
    conv_table = jnp.concatenate([conv_inner, conv_pair.reshape(CONV_TAPS, -1)], axis=1).astype(jnp.float32)
    half_taps = CONV_TAPS // 2
    rimmed = jnp.pad(carried_in, ((half_taps, half_taps), (0, 0)))
    filtered = rimmed[0:seq_total] * conv_table[0]
    for offset in range(1, CONV_TAPS):
        filtered = filtered + rimmed[offset:offset + seq_total] * conv_table[offset]
    activated = jax.nn.silu(filtered)
    map_width = SSM_GROUPS * STATE_SIZE
    signal = activated[:, :SSM_INNER].reshape(seq_total, SSM_GROUPS, ssm_ratio, HEAD_SIZE)
    in_state = activated[:, SSM_INNER:SSM_INNER + map_width].reshape(seq_total, SSM_GROUPS, STATE_SIZE)
    out_state = activated[:, SSM_INNER + map_width:].reshape(seq_total, SSM_GROUPS, STATE_SIZE)
    step_rows = project(step_weight.reshape(MODEL_WIDTH, 2 * DUALITY_CHANNELS))
    step = jax.nn.softplus(step_rows.astype(jnp.float32)).reshape(seq_total, 2, SSM_GROUPS, ssm_ratio)
    log_decay = -decay_rate.reshape(2, SSM_GROUPS, ssm_ratio) * step + decay_jump.reshape(seq_total, 2, SSM_GROUPS, ssm_ratio)
    forward_y = ssd_pass(signal * step[:, 0, :, :, None], log_decay[:, 0], in_state, out_state)
    backward_y = jnp.flip(ssd_pass(jnp.flip(signal * step[:, 1, :, :, None], 0), jnp.flip(log_decay[:, 1], 0), jnp.flip(in_state, 0), jnp.flip(out_state, 0)), 0)
    combined = (forward_y + backward_y).reshape(seq_total, SSM_INNER) * jax.nn.silu(gate_rows.astype(jnp.float32))
    grouped = rms_rows(combined.reshape(seq_total, SSM_GROUPS, -1), 1.0).reshape(seq_total, SSM_INNER)
    ssm_out = (grouped * inner_gain.astype(jnp.float32)).astype(jnp.bfloat16)
    attn_group = QUERY_HEADS * HEAD_SIZE // N_TP
    ssm_group = SSM_INNER // N_TP
    summed = jnp.zeros((seq_total, MODEL_WIDTH), jnp.float32)
    for group_index in range(N_TP):
        attn_cols = attn_out[:, group_index * attn_group:(group_index + 1) * attn_group]
        ssm_cols = ssm_out[:, group_index * ssm_group:(group_index + 1) * ssm_group]
        partial_sum = jnp.dot(attn_cols, attn_out_weight[group_index * attn_group:(group_index + 1) * attn_group], preferred_element_type=jnp.float32)
        partial_sum = partial_sum + jnp.dot(ssm_cols, ssm_out_weight[group_index * ssm_group:(group_index + 1) * ssm_group], preferred_element_type=jnp.float32)
        rounded = lax.optimization_barrier(partial_sum.astype(jnp.bfloat16))
        summed = summed + rounded.astype(jnp.float32)
    return summed.astype(jnp.bfloat16)
```

```python
import functools

import jax
import jax.numpy as jnp
from jax import lax
from jax.experimental import pallas as pl
from jax.experimental.pallas import tpu as pltpu
from jax.sharding import PartitionSpec as P

STATE_SIZE = 128
WINDOW = 128
CHUNK = 128
HALO = 16

NORM_EPS = 1e-05
ROPE_BASE = 500000.0
NEG_FILL = -1e30


def extended(block, sides, width):
    for axis, dim in sides:
        count = lax.axis_size(axis)
        forward = [(i, i + 1) for i in range(count - 1)]
        backward = [(target, source) for source, target in forward]
        low = lax.ppermute(
            lax.slice_in_dim(block, block.shape[dim] - width, None, axis=dim), axis, forward
        )
        high = lax.ppermute(lax.slice_in_dim(block, 0, width, axis=dim), axis, backward)
        block = jnp.concatenate([low, block, high], axis=dim)
    return block


def rms_rows(values, scales):
    return values * lax.rsqrt(jnp.mean(values * values, axis=-1, keepdims=True) + NORM_EPS) * scales


def rotate(head_rows, positions):
    head_size = head_rows.shape[-1]
    half_size = head_size // 2
    frequency = ROPE_BASE ** (-jnp.arange(0, head_size, 2, dtype=jnp.float32) / head_size)
    angles = positions.astype(jnp.float32)[:, None] * frequency
    cosine = jnp.cos(angles)[:, None, :]
    sine_part = jnp.sin(angles)[:, None, :]
    first_half = head_rows[..., :half_size]
    second_half = head_rows[..., half_size:]
    return jnp.concatenate(
        [
            first_half * cosine - second_half * sine_part,
            second_half * cosine + first_half * sine_part,
        ],
        axis=-1,
    )


def spread(factor, width):
    heads = factor.shape[1]
    row = lax.broadcasted_iota(jnp.int32, (heads, width), 0)
    column = lax.broadcasted_iota(jnp.int32, (heads, width), 1)
    head_size = width // heads
    ones = jnp.where(
        (column >= row * head_size) & (column < (row + 1) * head_size), 1.0, 0.0
    ).astype(jnp.bfloat16)
    return jnp.dot(factor.astype(jnp.bfloat16), ones, preferred_element_type=jnp.float32)


def exact_dot(a, b):
    return jnp.dot(a, b, precision=lax.Precision.HIGHEST, preferred_element_type=jnp.float32)


def triangle(size, lower):
    row = lax.broadcasted_iota(jnp.int32, (size, size), 0)
    column = lax.broadcasted_iota(jnp.int32, (size, size), 1)
    return jnp.where(row >= column if lower else row <= column, 1.0, 0.0)


def states_kernel(
    tap_count, inner, maps, rows_ref, taps_ref, ldf_ref, ldb_ref, stf_ref, stb_ref,
    act_ref, freshf_ref, freshb_ref, endf_ref, endb_ref, spare, reach,
):
    step = pl.program_id(0)
    size = act_ref.shape[0]
    start = pl.multiple_of(step * size, size)
    spare[...] = rows_ref[pl.ds(start, size + 2 * HALO), :].astype(jnp.float32)
    first = HALO - tap_count // 2
    filtered = spare[first : first + size, :] * taps_ref[0:1, :]
    for k in range(1, tap_count):
        filtered = filtered + spare[first + k : first + k + size, :] * taps_ref[k : k + 1, :]
    activated = filtered / (1.0 + jnp.exp(-filtered))
    act_ref[...] = activated.astype(jnp.bfloat16)
    signal = activated[:, :inner]
    ldf, ldb = ldf_ref[...], ldb_ref[...]
    cumf = exact_dot(triangle(size, True), ldf)
    cumb = exact_dot(triangle(size, False), ldb)
    wf = jnp.exp(cumf[size - 1 : size] - cumf) * stf_ref[...]
    wb = jnp.exp(cumb[0:1] - cumb) * stb_ref[...]
    xf = (signal * spread(wf, inner)).astype(jnp.bfloat16)
    xb = (signal * spread(wb, inner)).astype(jnp.bfloat16)
    totf = spread(jnp.exp(jnp.broadcast_to(cumf[size - 1 : size], (8, ldf.shape[1]))), inner)[0:1]
    totb = spread(jnp.exp(jnp.broadcast_to(cumb[0:1], (8, ldb.shape[1]))), inner)[0:1]

    @pl.when(step == 0)
    def _():
        endf_ref[...] = jnp.zeros_like(endf_ref)
        endb_ref[...] = jnp.zeros_like(endb_ref)
        reach[...] = jnp.ones_like(reach)

    groups = maps // STATE_SIZE
    width = inner // groups
    for g in range(groups):
        entry = activated[:, inner + g * STATE_SIZE : inner + (g + 1) * STATE_SIZE]
        entry = jnp.transpose(entry).astype(jnp.bfloat16)
        cols = slice(g * width, (g + 1) * width)
        ff = jnp.dot(entry, xf[:, cols], preferred_element_type=jnp.float32)
        fb = jnp.dot(entry, xb[:, cols], preferred_element_type=jnp.float32)
        freshf_ref[0, :, cols] = ff
        freshb_ref[0, :, cols] = fb
        endf_ref[:, cols] = endf_ref[:, cols] * totf[:, cols] + ff
        endb_ref[:, cols] = endb_ref[:, cols] + reach[0:1, cols] * fb
    reach[...] = reach[...] * totb


def outputs_kernel(
    head_size, inner, maps, act_ref, ldf_ref, ldb_ref, stf_ref, stb_ref, ldft_ref, ldbt_ref,
    stft_ref, stbt_ref, ldball_ref, freshf_ref, freshb_ref, inf_ref, inb_ref, gate_ref, gain_ref,
    out_ref, carryf, enterb, y,
):
    step = pl.program_id(0)
    chunks = pl.num_programs(0)
    size = act_ref.shape[0]
    heads = inner // head_size

    @pl.when(step == 0)
    def _():
        carryf[...] = inf_ref[...]
        enterb[chunks - 1] = inb_ref[...]

        @pl.loop(0, chunks - 1)
        def _(k):
            at = chunks - 1 - k
            part = ldball_ref[pl.ds(pl.multiple_of(at * size, size), size), :]
            tot = jnp.exp(jnp.sum(part, axis=0, keepdims=True))
            tot = spread(jnp.broadcast_to(tot, (8, heads)), inner)[0:1]
            enterb[at - 1] = enterb[at] * tot + freshb_ref[at]

    lower, upper = triangle(size, True), triangle(size, False)
    cumf = exact_dot(lower, ldf_ref[...])
    cumb = exact_dot(upper, ldb_ref[...])
    cumft = exact_dot(ldft_ref[...], upper)
    cumbt = exact_dot(ldbt_ref[...], lower)
    stft, stbt = stft_ref[...], stbt_ref[...]
    row = lax.broadcasted_iota(jnp.int32, (size, size), 0)
    column = lax.broadcasted_iota(jnp.int32, (size, size), 1)
    is_lower, is_diagonal = row >= column, row == column
    groups = maps // STATE_SIZE
    width = inner // groups
    group_heads = heads // groups
    expf = spread(jnp.exp(cumf), inner)
    expb = spread(jnp.exp(cumb), inner)
    lane = lax.broadcasted_iota(jnp.int32, (size, 2 * head_size), 1)
    for g in range(groups):
        cols = slice(g * width, (g + 1) * width)
        entry = act_ref[:, inner + g * STATE_SIZE : inner + (g + 1) * STATE_SIZE]
        leave = act_ref[:, inner + maps + g * STATE_SIZE : inner + maps + (g + 1) * STATE_SIZE]
        crossed = lax.dot_general(
            leave, entry, (((1,), (1,)), ((), ())), preferred_element_type=jnp.float32
        )
        y[:, cols] = (
            jnp.dot(leave, carryf[:, cols].astype(jnp.bfloat16), preferred_element_type=jnp.float32)
            * expf[:, cols]
            + jnp.dot(
                leave, enterb[step, :, cols].astype(jnp.bfloat16),
                preferred_element_type=jnp.float32,
            )
            * expb[:, cols]
        )
        for pair in range(group_heads // 2):
            mats = []
            base = g * group_heads + 2 * pair
            for h in (base, base + 1):
                gap = jnp.where(
                    is_lower,
                    cumf[:, h : h + 1] - cumft[h : h + 1, :],
                    cumb[:, h : h + 1] - cumbt[h : h + 1, :],
                )
                sf, sb = stft[h : h + 1, :], stbt[h : h + 1, :]
                amount = jnp.where(is_diagonal, sf + sb, jnp.where(is_lower, sf, sb))
                mats.append((crossed * jnp.exp(gap) * amount).astype(jnp.bfloat16))
            two = slice(base * head_size, (base + 2) * head_size)
            x = act_ref[:, two]
            zero = jnp.zeros_like(x)
            stacked = jnp.concatenate(
                [jnp.where(lane < head_size, x, zero), jnp.where(lane < head_size, zero, x)], axis=0
            )
            y[:, two] += jnp.dot(
                jnp.concatenate(mats, axis=1), stacked, preferred_element_type=jnp.float32
            )
        gate = gate_ref[:, cols].astype(jnp.float32)
        mixed = y[:, cols] * (gate / (1.0 + jnp.exp(-gate)))
        scale = lax.rsqrt(jnp.mean(mixed * mixed, axis=1, keepdims=True) + NORM_EPS)
        out_ref[:, cols] = (mixed * scale * gain_ref[:, cols]).astype(jnp.bfloat16)
    totf = spread(jnp.exp(jnp.broadcast_to(cumf[size - 1 : size], (8, heads))), inner)[0:1]
    carryf[...] = carryf[...] * totf + freshf_ref[0]


def attend_kernel(head_size, key_heads, place_ref, sink_ref, query_ref, rim_ref, out_ref):
    step = pl.program_id(0)
    size = query_ref.shape[0]
    reach = size + 2 * WINDOW
    heads = query_ref.shape[1] // head_size
    ratio = heads // key_heads
    start = pl.multiple_of(step * size, size)
    row = lax.broadcasted_iota(jnp.int32, (size, reach), 0)
    column = lax.broadcasted_iota(jnp.int32, (size, reach), 1)
    key_pos = place_ref[0] + step * size - WINDOW + column
    allowed = (
        (column >= row) & (column <= row + 2 * WINDOW) & (key_pos >= 0) & (key_pos < place_ref[1])
    )
    scale = head_size ** (-0.5)
    for k in range(key_heads):
        keys = rim_ref[pl.ds(start, reach), k * head_size : (k + 1) * head_size]
        values = rim_ref[
            pl.ds(start, reach), (key_heads + k) * head_size : (key_heads + k + 1) * head_size
        ]
        for r in range(ratio):
            h = k * ratio + r
            cols = slice(h * head_size, (h + 1) * head_size)
            scores = lax.dot_general(
                query_ref[:, cols], keys, (((1,), (1,)), ((), ())),
                preferred_element_type=jnp.float32,
            )
            scores = jnp.where(allowed, scores * scale, NEG_FILL)
            sink = sink_ref[h]
            ceiling = jnp.maximum(jnp.max(scores, axis=1, keepdims=True), sink)
            raised = jnp.exp(scores - ceiling)
            bottom = jnp.sum(raised, axis=1, keepdims=True) + jnp.exp(sink - ceiling)
            weights = (raised * (1.0 / bottom)).astype(jnp.bfloat16)
            out_ref[:, cols] = jnp.dot(
                weights, values, preferred_element_type=jnp.float32
            ).astype(jnp.bfloat16)


def attend(query, rimmed, sink_logit, seq_first, seq_total, head_size, key_heads):
    rows, width = query.shape
    block = WINDOW
    place = jnp.stack([jnp.int32(seq_first), jnp.int32(seq_total)])
    return pl.pallas_call(
        functools.partial(attend_kernel, head_size, key_heads),
        grid=(rows // block,),
        in_specs=[
            pl.BlockSpec(memory_space=pltpu.SMEM),
            pl.BlockSpec(memory_space=pltpu.SMEM),
            pl.BlockSpec((block, width), lambda i: (i, 0)),
            pl.BlockSpec(rimmed.shape, lambda i: (0, 0)),
        ],
        out_specs=pl.BlockSpec((block, width), lambda i: (i, 0)),
        out_shape=jax.ShapeDtypeStruct((rows, width), jnp.bfloat16),
        cost_estimate=pl.CostEstimate(
            flops=4 * rows * 3 * WINDOW * width, bytes_accessed=4 * rows * width,
            transcendentals=rows * 3 * WINDOW * width // head_size,
        ),
        name="attend",
    )(place, sink_logit, query, rimmed)


def chunk_states(rimmed, taps, tap_count, inner, maps, decay, step):
    rows = rimmed.shape[0] - 2 * HALO
    total, heads, chunks = rimmed.shape[1], decay[0].shape[1], rows // CHUNK
    small = pl.BlockSpec((CHUNK, heads), lambda i: (i, 0))
    fresh = pl.BlockSpec((1, STATE_SIZE, inner), lambda i: (i, 0, 0))
    end = pl.BlockSpec((STATE_SIZE, inner), lambda i: (0, 0))
    fresh_shape = jax.ShapeDtypeStruct((chunks, STATE_SIZE, inner), jnp.float32)
    end_shape = jax.ShapeDtypeStruct((STATE_SIZE, inner), jnp.float32)
    return pl.pallas_call(
        functools.partial(states_kernel, tap_count, inner, maps),
        grid=(chunks,),
        in_specs=[
            pl.BlockSpec(rimmed.shape, lambda i: (0, 0)),
            pl.BlockSpec(taps.shape, lambda i: (0, 0)),
            small, small, small, small,
        ],
        out_specs=[pl.BlockSpec((CHUNK, total), lambda i: (i, 0)), fresh, fresh, end, end],
        out_shape=[
            jax.ShapeDtypeStruct((rows, total), jnp.bfloat16),
            fresh_shape, fresh_shape, end_shape, end_shape,
        ],
        scratch_shapes=[
            pltpu.VMEM((CHUNK + 2 * HALO, total), jnp.float32),
            pltpu.VMEM((8, inner), jnp.float32),
        ],
        cost_estimate=pl.CostEstimate(
            flops=8 * rows * inner * STATE_SIZE, bytes_accessed=16 * rows * inner,
            transcendentals=rows * total,
        ),
        name="chunk_states",
    )(rimmed, taps, *decay, *step)


def chunk_outputs(head_size, inner, maps, act, decay, step, fresh, incoming, gate, gain):
    rows, total = act.shape
    heads, chunks = decay[0].shape[1], rows // CHUNK
    small = pl.BlockSpec((CHUNK, heads), lambda i: (i, 0))
    turned = pl.BlockSpec((heads, CHUNK), lambda i: (0, i))
    whole = pl.BlockSpec((STATE_SIZE, inner), lambda i: (0, 0))
    return pl.pallas_call(
        functools.partial(outputs_kernel, head_size, inner, maps),
        grid=(chunks,),
        in_specs=[
            pl.BlockSpec((CHUNK, total), lambda i: (i, 0)),
            small, small, small, small, turned, turned, turned, turned,
            pl.BlockSpec((rows, heads), lambda i: (0, 0)),
            pl.BlockSpec((1, STATE_SIZE, inner), lambda i: (i, 0, 0)),
            pl.BlockSpec((chunks, STATE_SIZE, inner), lambda i: (0, 0, 0)),
            whole, whole,
            pl.BlockSpec((CHUNK, inner), lambda i: (i, 0)),
            pl.BlockSpec((1, inner), lambda i: (0, 0)),
        ],
        out_specs=pl.BlockSpec((CHUNK, inner), lambda i: (i, 0)),
        out_shape=jax.ShapeDtypeStruct((rows, inner), jnp.bfloat16),
        scratch_shapes=[
            pltpu.VMEM((STATE_SIZE, inner), jnp.float32),
            pltpu.VMEM((chunks, STATE_SIZE, inner), jnp.float32),
            pltpu.VMEM((CHUNK, inner), jnp.float32),
        ],
        cost_estimate=pl.CostEstimate(
            flops=8 * rows * inner * STATE_SIZE, bytes_accessed=16 * rows * inner,
            transcendentals=rows * CHUNK * heads,
        ),
        name="chunk_outputs",
    )(
        act, *decay, *step, decay[0].T, decay[1].T, step[0].T, step[1].T, decay[1],
        fresh[0], fresh[1], incoming[0], incoming[1], gate, gain,
    )


def entering_state(end, total, axis, head_size, reverse):
    count = lax.axis_size(axis)
    states = end.shape[0]

    def moved(packet, distance):
        pairs = [(i, i + distance) for i in range(count - distance)]
        if reverse:
            pairs = [(target, source) for source, target in pairs]
        return lax.ppermute(packet, axis, pairs)

    decay = jnp.broadcast_to(jnp.repeat(jnp.exp(total), head_size)[None, :], (16, end.shape[1]))
    packet = jnp.concatenate([end, decay], axis=0).astype(jnp.bfloat16)
    packet = moved(packet, 1)
    distance = 1
    held = packet.astype(jnp.float32)
    while distance < count - 1:
        arrived = moved(held.astype(jnp.bfloat16), distance).astype(jnp.float32)
        factor = held[states : states + 1]
        added = jnp.concatenate([held[:states], jnp.zeros_like(held[states:])], axis=0)
        held = added + factor * arrived
        distance *= 2
    return held[:states]


def local(
    tokens,
    norm_gain,
    query_weight,
    key_weight,
    value_weight,
    query_gain,
    key_gain,
    sink_logit,
    gate_weight,
    inner_weight,
    input_map,
    output_map,
    step_weight,
    conv_inner,
    conv_pair,
    decay_rate,
    decay_jump,
    inner_gain,
    attn_out_weight,
    ssm_out_weight,
):
    row_total = tokens.shape[0]
    seq_total = row_total * lax.axis_size("sp")
    seq_first = lax.axis_index("sp") * row_total
    positions = seq_first + jnp.arange(row_total, dtype=jnp.int32)
    normed = rms_rows(tokens.astype(jnp.float32), norm_gain.astype(jnp.float32)).astype(
        jnp.bfloat16
    )

    def project(weight):
        result = jnp.dot(normed, weight, preferred_element_type=jnp.float32)
        return lax.optimization_barrier(result.astype(jnp.bfloat16))

    head_size = query_gain.shape[0]
    query = project(query_weight).reshape(row_total, -1, head_size)
    keyed = project(key_weight).reshape(row_total, -1, head_size)
    value = project(value_weight)
    query = rotate(rms_rows(query.astype(jnp.float32), query_gain), positions).astype(jnp.bfloat16)
    keyed = rotate(rms_rows(keyed.astype(jnp.float32), key_gain), positions).astype(jnp.bfloat16)
    key_heads = keyed.shape[1]
    packed = jnp.concatenate([keyed.reshape(row_total, -1), value], axis=1)
    rimmed_keys = extended(packed, (("sp", 0),), WINDOW)
    inner_rows = project(inner_weight)
    inner_width = inner_rows.shape[1]
    map_width = input_map.shape[1]
    carried_in = jnp.concatenate([inner_rows, project(input_map), project(output_map)], axis=1)
    tap_count = conv_inner.shape[0]
    conv_table = jnp.concatenate([conv_inner, conv_pair.reshape(tap_count, -1)], axis=1).astype(
        jnp.float32
    )
    rimmed_rows = extended(carried_in, (("sp", 0),), HALO)
    step_rows = project(step_weight.reshape(step_weight.shape[0], -1))
    step = jax.nn.softplus(step_rows.astype(jnp.float32))
    log_decay = -decay_rate.reshape(1, -1) * step + decay_jump.reshape(row_total, -1)
    heads_here = inner_width // head_size
    steps = (step[:, :heads_here], step[:, heads_here:])
    decays = (log_decay[:, :heads_here], log_decay[:, heads_here:])
    act, fresh_forward, fresh_backward, end_forward, end_backward = chunk_states(
        rimmed_rows, conv_table, tap_count, inner_width, map_width, decays, steps
    )
    from_lower = entering_state(end_forward, jnp.sum(decays[0], axis=0), "sp", head_size, False)
    from_higher = entering_state(end_backward, jnp.sum(decays[1], axis=0), "sp", head_size, True)
    attn_out = attend(
        query.reshape(row_total, -1), rimmed_keys, sink_logit, seq_first, seq_total, head_size,
        key_heads,
    )
    gate_rows = project(gate_weight)
    ssm_out = chunk_outputs(
        head_size, inner_width, map_width, act, decays, steps, (fresh_forward, fresh_backward),
        (from_lower, from_higher), gate_rows, inner_gain.astype(jnp.float32)[None, :],
    )
    partial_sum = jnp.dot(attn_out, attn_out_weight, preferred_element_type=jnp.float32)
    partial_sum = partial_sum + jnp.dot(ssm_out, ssm_out_weight, preferred_element_type=jnp.float32)
    rounded = lax.optimization_barrier(partial_sum.astype(jnp.bfloat16))
    return lax.psum_scatter(
        rounded.astype(jnp.float32).astype(jnp.bfloat16), "tp", scatter_dimension=0, tiled=True
    )


def solution(mesh):
    in_specs = (
        P("sp", None),
        P(),
        P(None, "tp"),
        P(None, "tp"),
        P(None, "tp"),
        P(),
        P(),
        P("tp"),
        P(None, "tp"),
        P(None, "tp"),
        P(None, "tp"),
        P(None, "tp"),
        P(None, None, "tp"),
        P(None, "tp"),
        P(None, None, "tp"),
        P(None, "tp"),
        P("sp", None, "tp"),
        P("tp"),
        P("tp", None),
        P("tp", None),
    )
    out_specs = P(("sp", "tp"), None)
    return jax.shard_map(local, mesh=mesh, in_specs=in_specs, out_specs=out_specs, check_vma=False)
```
